32 devices in a mesh: sp: 8 (over z, x), tp: 4 (over y, core).
Axes of the slice: x: 2, y: 2, z: 4, core: 2. Of those that a mesh axis runs over, the one named last changes fastest.
Arguments:
- queries: bfloat16 [8192, 1536], P('sp', 'tp'), may hold values from -200 to 200
- key_heads: bfloat16 [8192, 512], P('sp', 'tp'), may hold values from -6 to 6
- projected_value_heads: bfloat16 [8192, 512], P('sp', 'tp'), may hold values from -5 to 5
- sink_logit_table: float32 [24], P('tp'), may hold values from 0 to 4
- out_weight: bfloat16 [1536, 3072], P('tp'), may hold values from -1.5 to 1.5
- residual: bfloat16 [8192, 3072], P('sp', 'tp'), may hold values from -16 to 16
- norm_gain: bfloat16 [3072], P('tp'), may hold values from 0.099609375 to 1.8984375
- up_weight: bfloat16 [3072, 12288], P('sp', 'tp'), may hold values from -0.109375 to 0.109375
- down_weight: bfloat16 [12288, 3072], P('tp', 'sp'), may hold values from -0.0546875 to 0.0546875
Outputs:
- result: bfloat16 [8192, 3072], P('sp', 'tp')
The draws below stay inside these ranges and needn't reach their ends.
All inputs are finite; a program needn't handle non-finite values.
Results may differ from the reference program's by a relative error of at most 0.015.
Values may be sent and summed in bfloat16 or wider, within the bound.
No kernel may reach another device: no remote copies, remote signals or barrier semaphores. Data moves between devices by JAX's collectives and lax.ppermute only.
A program may use at most 128 MiB of HBM per device.

```python
import math
import jax
import jax.numpy as jnp
from jax import lax

D = 3072
FF = 12288
QUERY_HEADS = 24
KEY_VALUE_HEADS = 8
HEAD_SIZE = 64
WINDOW_SPAN = 128
SEQUENCE_TOKENS = 8192
N_TP = 4


def inserted_value(key):
    starting_query = jax.random.truncated_normal(jax.random.fold_in(key, 11), -5.0, 5.0, (SEQUENCE_TOKENS, KEY_VALUE_HEADS, QUERY_HEADS // KEY_VALUE_HEADS, HEAD_SIZE), jnp.float32)
    starting_keys = jax.random.truncated_normal(jax.random.fold_in(key, 12), -5.0, 5.0, (SEQUENCE_TOKENS, KEY_VALUE_HEADS, HEAD_SIZE), jnp.float32)
    query_out = starting_query
    keys_out = starting_keys
    return (query_out, keys_out)


def draw_queries(key, part):
    return inserted_value(key)[0].reshape(SEQUENCE_TOKENS, QUERY_HEADS * HEAD_SIZE).astype(jnp.bfloat16)


def draw_key_heads(key, part):
    return inserted_value(key)[1].reshape(SEQUENCE_TOKENS, KEY_VALUE_HEADS * HEAD_SIZE).astype(jnp.bfloat16)


def draw_residual(key, part):
    column = jnp.arange(D).astype(jnp.float32) / (D - 1)
    base = jax.random.truncated_normal(jax.random.fold_in(key, 22), -5.0, 5.0, (SEQUENCE_TOKENS, D), jnp.float32)
    scale = jnp.exp(math.log(3.0) * column)
    return (base * scale[None, :]).astype(jnp.bfloat16)


def shard_levels(rng, dims, split, low, largest):
    def one(position, shards_of):
        steps = jax.random.uniform(jax.random.fold_in(jax.random.fold_in(rng, 6), position), (shards_of,), jnp.float32, low / len(split), largest / len(split))
        return jnp.repeat(jnp.exp(steps), dims[position] // shards_of).reshape((-1,) + (1,) * (len(dims) - position - 1))

    loudness = one(*split[0])
    for cut in split[1:]:
        loudness = loudness * one(*cut)
    return loudness


def noise(stream_key, shape, width, reach, split=(), kind=jnp.bfloat16):
    values = jax.random.normal(stream_key, shape, jnp.float32) * width
    if len(split) > 0:
        values = shard_levels(stream_key, shape, split, -0.22, 0.18) * values
    return jnp.clip(values, min=-reach, max=reach).astype(kind)


def setup_inputs(seed: int = 0) -> dict:
    keys = jax.random.split(jax.random.key(seed), 10)
    queries = draw_queries(jax.random.fold_in(keys[9], 71), 0)
    key_heads = draw_key_heads(jax.random.fold_in(keys[9], 71), 0)
    projected_value_heads = noise(keys[2], (SEQUENCE_TOKENS, KEY_VALUE_HEADS * HEAD_SIZE), 1.0, 5.0, ((0, 8), (1, 4)))
    sink_logit_table = jnp.clip(4.0 * jax.random.uniform(keys[3], (QUERY_HEADS,), jnp.float32) ** shard_levels(keys[3], (QUERY_HEADS,), ((0, 4),), -0.2, 0.2), 0.0, 4.0)
    out_weight = noise(keys[4], (QUERY_HEADS * HEAD_SIZE, D), 0.25, 1.5, ((0, 4),))
    residual = draw_residual(jax.random.fold_in(keys[9], 71), 0)
    norm_gain = jnp.clip(1.0 + 0.18 * jax.random.normal(keys[6], (D,), jnp.float32), 0.099609375, 1.8984375).astype(jnp.bfloat16)
    up_weight = noise(keys[7], (D, FF), D ** -0.5, 0.109375, ((0, 8), (1, 4)))
    down_weight = noise(keys[8], (FF, D), FF ** -0.5, 0.0546875, ((0, 4), (1, 8)))
    return dict(queries=queries, key_heads=key_heads, projected_value_heads=projected_value_heads, sink_logit_table=sink_logit_table, out_weight=out_weight, residual=residual, norm_gain=norm_gain, up_weight=up_weight, down_weight=down_weight)


epsilon = 1e-06

def attend(queries, key_heads, projected_value_heads, sink_logit_table):
    sequence_length = queries.shape[0]
    block_count = sequence_length // WINDOW_SPAN
    group_count = QUERY_HEADS // KEY_VALUE_HEADS
    query_block_list = queries.astype(jnp.float32).reshape(block_count, WINDOW_SPAN, KEY_VALUE_HEADS, group_count, HEAD_SIZE)

    def banded(source_rows):
        padded_rows = jnp.pad(source_rows.astype(jnp.float32).reshape(sequence_length, KEY_VALUE_HEADS, HEAD_SIZE), ((WINDOW_SPAN, 0), (0, 0), (0, 0)))
        padded_rows = padded_rows.reshape(block_count + 1, WINDOW_SPAN, KEY_VALUE_HEADS, HEAD_SIZE)
        return jnp.concatenate([padded_rows[:-1], padded_rows[1:]], axis=1)
    key_band = banded(key_heads)
    value_band = banded(projected_value_heads)
    scores = jnp.einsum('nqkgd,nskd->nkgqs', query_block_list, key_band) * HEAD_SIZE ** (-0.5)
    within = jnp.arange(WINDOW_SPAN)[:, None]
    column = jnp.arange(2 * WINDOW_SPAN)[None, :]
    distance = WINDOW_SPAN + within - column
    valid = (distance >= 0) & (distance < WINDOW_SPAN)
    key_pos = jnp.arange(block_count)[:, None] * WINDOW_SPAN + jnp.arange(2 * WINDOW_SPAN)[None, :] - WINDOW_SPAN
    allowed = valid[None] & (key_pos >= 0)[:, None, :]
    allowed = allowed[:, None, None]
    head_sink_logit = sink_logit_table.astype(jnp.float32).reshape(KEY_VALUE_HEADS, group_count)[None, :, :, None, None]
    masked = jnp.where(allowed, scores, -1e+30)
    ceiling = jnp.maximum(lax.optimization_barrier(jnp.max(masked, axis=-1, keepdims=True)), head_sink_logit)
    powers = jnp.where(allowed, jnp.exp(masked - ceiling), 0.0)
    denom = lax.optimization_barrier(jnp.sum(powers, axis=-1, keepdims=True)) + jnp.exp(head_sink_logit - ceiling)
    probs = (powers / denom).astype(jnp.bfloat16)
    output = jnp.einsum('nkgqs,nskd->nqkgd', probs.astype(jnp.float32), value_band)
    return output.reshape(sequence_length, QUERY_HEADS * HEAD_SIZE).astype(jnp.bfloat16)

def reference(queries, key_heads, projected_value_heads, sink_logit_table, out_weight, residual, norm_gain, up_weight, down_weight):
    attended = attend(queries, key_heads, projected_value_heads, sink_logit_table)
    head_cols = QUERY_HEADS * HEAD_SIZE // N_TP
    mixed = jnp.zeros(residual.shape, jnp.float32)
    for group in range(N_TP):
        part = jnp.dot(attended[:, group * head_cols:(group + 1) * head_cols], out_weight[group * head_cols:(group + 1) * head_cols], preferred_element_type=jnp.float32)
        part = lax.optimization_barrier(part.astype(jnp.bfloat16))
        mixed = mixed + part.astype(jnp.float32)
    stream = lax.optimization_barrier((residual.astype(jnp.float32) + mixed).astype(jnp.bfloat16)).astype(jnp.float32)
    mean_square = lax.optimization_barrier(jnp.mean(stream * stream, axis=-1, keepdims=True)) + epsilon
    normed = (stream * lax.rsqrt(mean_square) * norm_gain.astype(jnp.float32)).astype(jnp.bfloat16)
    unit_cols = FF // N_TP
    branch_sum = jnp.zeros(residual.shape, jnp.float32)
    for group in range(N_TP):
        hidden_pre = jnp.dot(normed, up_weight[:, group * unit_cols:(group + 1) * unit_cols], preferred_element_type=jnp.float32)
        activated = jnp.square(jax.nn.relu(hidden_pre)).astype(jnp.bfloat16)
        branch = jnp.dot(activated, down_weight[group * unit_cols:(group + 1) * unit_cols], preferred_element_type=jnp.float32)
        branch = lax.optimization_barrier(branch.astype(jnp.bfloat16))
        branch_sum = branch_sum + branch.astype(jnp.float32)
    return (stream + branch_sum).astype(jnp.bfloat16)
```

```python
import jax
import jax.numpy as jnp
from jax import lax
from jax.sharding import PartitionSpec as P


D = 3072
HEAD_SIZE = 64
WINDOW_SPAN = 128


epsilon = 1e-06


def shifted(block, axis, distance):
    devices = range(lax.axis_size(axis))
    route = [(i - distance, i) for i in devices if i - distance in devices]
    return lax.ppermute(block, axis, route)


def attend(queries, key_heads, projected_value_heads, sink_logit_table, previous, offset):
    row_count = queries.shape[0]
    kv_cols = key_heads.shape[1]
    kv_local = kv_cols // HEAD_SIZE
    group_count = queries.shape[1] // kv_cols
    block_count = row_count // WINDOW_SPAN
    extended_keys = jnp.concatenate([previous[:, :kv_cols], key_heads], axis=0)
    extended_values = jnp.concatenate([previous[:, kv_cols:], projected_value_heads], axis=0)

    def banded(source_rows):
        shaped = source_rows.reshape(block_count + 1, WINDOW_SPAN, kv_local, HEAD_SIZE)
        return jnp.concatenate([shaped[:-1], shaped[1:]], axis=1)

    key_band = banded(extended_keys)
    value_band = banded(extended_values)
    query_block_list = queries.reshape(block_count, WINDOW_SPAN, kv_local, group_count, HEAD_SIZE)
    scores = jnp.einsum(
        "nqkgd,nskd->nkgqs", query_block_list, key_band, preferred_element_type=jnp.float32
    )
    scores = scores * HEAD_SIZE ** (-0.5)
    within = jnp.arange(WINDOW_SPAN)[:, None]
    column = jnp.arange(2 * WINDOW_SPAN)[None, :]
    distance = WINDOW_SPAN + within - column
    valid = (distance >= 0) & (distance < WINDOW_SPAN)
    key_pos = (
        offset
        + jnp.arange(block_count)[:, None] * WINDOW_SPAN
        + jnp.arange(2 * WINDOW_SPAN)[None, :]
        - WINDOW_SPAN
    )
    allowed = valid[None] & (key_pos >= 0)[:, None, :]
    allowed = allowed[:, None, None]
    head_sink_logit = sink_logit_table.reshape(kv_local, group_count)[None, :, :, None, None]
    masked = jnp.where(allowed, scores, -1e30)
    ceiling = jnp.maximum(jnp.max(masked, axis=-1, keepdims=True), head_sink_logit)
    powers = jnp.where(allowed, jnp.exp(masked - ceiling), 0.0)
    denom = jnp.sum(powers, axis=-1, keepdims=True) + jnp.exp(head_sink_logit - ceiling)
    probs = (powers / denom).astype(jnp.bfloat16)
    output = jnp.einsum("nkgqs,nskd->nqkgd", probs, value_band, preferred_element_type=jnp.float32)
    return output.astype(jnp.bfloat16).reshape(row_count, queries.shape[1])


def loop_order(size):
    return list(range(0, size, 2)) + list(range(size - 1, 0, -2))


def walked(shard):
    size = lax.axis_size("sp")
    order = loop_order(size)
    ahead = [(order[i], order[(i + 1) % size]) for i in range(size)]
    behind = [(b, a) for a, b in ahead]

    def send(block, route):
        return lax.ppermute(block, "sp", route)

    middle = shard.shape[0] // 2
    above = below = shard
    blocks = []
    for step in range(1, size // 2):
        above, below = send(above, ahead), send(below, behind)
        blocks += [(-step, above), (step, below)]
    far = (send(above[:middle], ahead), send(below[middle:], behind))
    return blocks, far


def place():
    size = lax.axis_size("sp")
    index = lax.axis_index("sp")
    return jnp.where(index % 2 == 0, index // 2, size - 1 - index // 2)


def source(step):
    size = lax.axis_size("sp")
    spot = (place() + step) % size
    side = (spot >= size // 2).astype(jnp.int32)
    return jnp.where(side == 0, spot, size - 1 - spot), side


def rounded(values):
    return lax.optimization_barrier(values.astype(jnp.bfloat16)).astype(jnp.float32)


def body(
    queries,
    key_heads,
    projected_value_heads,
    sink_logit_table,
    out_weight,
    residual,
    norm_gain,
    up_weight,
    down_weight,
):
    row_count = queries.shape[0]
    offset = lax.axis_index("sp") * row_count
    up_blocks, up_far = walked(up_weight)
    down_blocks, down_far = walked(down_weight)
    tail = jnp.concatenate(
        [key_heads[row_count - WINDOW_SPAN :], projected_value_heads[row_count - WINDOW_SPAN :]],
        axis=1,
    )
    previous = shifted(tail, "sp", 1)
    attended = attend(queries, key_heads, projected_value_heads, sink_logit_table, previous, offset)
    partial_value = jnp.dot(attended, out_weight, preferred_element_type=jnp.float32)
    mixed_sum = lax.psum_scatter(
        partial_value.astype(jnp.bfloat16), "tp", scatter_dimension=1, tiled=True
    )
    mixed_sum = mixed_sum.astype(jnp.float32)
    stream = rounded(residual.astype(jnp.float32) + mixed_sum)
    squares = lax.psum(jnp.sum(stream * stream, axis=1, keepdims=True), "tp")
    normed = (stream * lax.rsqrt(squares / D + epsilon) * norm_gain.astype(jnp.float32)).astype(
        jnp.bfloat16
    )
    normed_whole = lax.all_gather(normed, "tp", axis=1, tiled=True)
    size = lax.axis_size("sp")
    column = lax.axis_index("sp") % 2
    rows = size // 2
    deep = up_weight.shape[0]
    wide = down_weight.shape[1]
    up_whole = jnp.zeros((size * deep, up_weight.shape[1]), up_weight.dtype)
    pieces = [(0, 0, up_weight)] + [(step, 0, block) for step, block in up_blocks]
    pieces += [(rows, 0, up_far[0]), (rows, deep // 2, up_far[1])]
    for step, top, block in pieces:
        row, side = source(step)
        start = (2 * row + side) * deep + top
        up_whole = lax.dynamic_update_slice(up_whole, block, (start, 0))
    hidden_pre = jnp.dot(normed_whole, up_whole, preferred_element_type=jnp.float32)
    activated = jnp.square(jax.nn.relu(hidden_pre)).astype(jnp.bfloat16)

    terms = jnp.zeros((size, row_count, wide), jnp.bfloat16)
    for step, block in [(0, down_weight)] + down_blocks:
        row, side = source(step)
        term = jnp.dot(activated, block, preferred_element_type=jnp.float32)
        at = jnp.where(side == column, row, rows + row)
        terms = lax.dynamic_update_slice(terms, term.astype(jnp.bfloat16)[None], (at, 0, 0))
    ours = lax.psum_scatter(terms[:rows], "tp", scatter_dimension=0, tiled=True)
    term = jnp.dot(activated, jnp.concatenate(down_far, axis=0), preferred_element_type=jnp.float32)
    second = lax.dynamic_update_slice(
        terms[rows:], term.astype(jnp.bfloat16)[None], (source(rows)[0], 0, 0)
    )
    theirs = lax.psum_scatter(second, "tp", scatter_dimension=0, tiled=True)
    low = jnp.where(column == 0, ours, theirs)
    high = jnp.where(column == 0, theirs, ours)
    branch_sum = jnp.stack([low, high], axis=1).reshape(-1, row_count, wide)
    branch_sum = branch_sum.transpose(1, 0, 2).reshape(row_count, -1).astype(jnp.float32)
    return (stream + branch_sum).astype(jnp.bfloat16)


def solution(mesh):
    return jax.shard_map(
        body,
        mesh=mesh,
        in_specs=(
            P("sp", "tp"),
            P("sp", "tp"),
            P("sp", "tp"),
            P("tp"),
            P("tp", None),
            P("sp", "tp"),
            P("tp"),
            P("sp", "tp"),
            P("tp", "sp"),
        ),
        out_specs=P("sp", "tp"),
        check_vma=False,
    )
```
